32 devices in a mesh: grp: 2 (over x), ep: 4 (over y, core), tp: 4 (over z).
Axes of the slice: x: 2, y: 2, z: 4, core: 2. Of those that a mesh axis runs over, the one named last changes fastest.
Arguments:
- tokens: bfloat16 [3072, 4096], P(('grp', 'ep'), 'tp'), parts along dimension 0
- pre_gain: float32 [4096], replicated, may hold values from 0.1 to 1.9
- out_gain: float32 [4096], P('tp'), may hold values from 0.1 to 1.9
- chosen: int32 [8, 4, 48], P(('grp', 'ep')), parts along dimension 0, may hold values from 0 to 383, as said below
- route_weight: float32 [8, 4, 48], P(('grp', 'ep')), parts along dimension 0, may hold values from 0.3 to 3
- expert_gate: bfloat16 [4, 4096, 3072], P('ep', None, 'tp'), may hold values from -0.09375 to 0.09375
- expert_up: bfloat16 [4, 4096, 3072], P('ep', None, 'tp'), may hold values from -0.09375 to 0.09375
- expert_down: bfloat16 [4, 3072, 4096], P('ep', 'tp'), may hold values from -0.109375 to 0.109375
Outputs:
- output: bfloat16 [3072, 4096], P(('grp', 'ep'), 'tp'), parts along dimension 0
The draws below stay inside these ranges and needn't reach their ends.
There are 2 independent parts, one for each index of `grp`. The reference program is written for one: setup_inputs(seed, part) draws one part's arguments, and reference() takes and returns one part's arrays. A program takes and returns all parts, laid end to end along the dimension named above; an argument that names none is the same for every part. Nothing has to cross between parts.
Inputs may be any that keep to these rules, and one draw needn't show every extreme that they name: chosen[b, e, k] is the position, within block b of 384 tokens, of the k-th token that expert e takes from that block; the 48 positions of one block and one expert are all different.
All inputs are finite; a program needn't handle non-finite values.
Results may differ from the reference program's by a relative error of at most 0.0075.
Values may be sent and summed in bfloat16 or wider, within the bound.
No kernel may reach another device: no remote copies, remote signals or barrier semaphores. Data moves between devices by JAX's collectives and lax.ppermute only.
A program may use at most 64 MiB of HBM per device.

```python
import math
import jax
import jax.numpy as jnp
from jax import lax

D = 4096
FF = 3072
TOK_DEV = 384
SLOT = 48
BLOCKS = 4
EXPERTS = 4
CAP = 192
TOKENS = 1536
N_TP = 4


def draw_tokens(key, part):
    key_base, key_rough, key_rows = jax.random.split(jax.random.fold_in(key, 11), 3)
    rough = jnp.exp(jax.random.uniform(key_rough, (D,), jnp.float32, -0.4, 0.4))
    row_scale = 0.5 * jnp.exp(jax.random.uniform(key_rows, (TOKENS, 1), jnp.float32, 0.0, math.log(10.0)))
    column_scale = jnp.exp(jnp.linspace(0.0, math.log(4.0), D, dtype=jnp.float32))
    base = jax.random.normal(key_base, (TOKENS, D), jnp.float32)
    return (base * column_scale * rough * row_scale).astype(jnp.bfloat16)


def draw_chosen(key, part):
    shape_all = (BLOCKS, EXPERTS, TOK_DEV)
    scores = jax.random.randint(jax.random.fold_in(key, 7), shape_all, 0, 1 << 20)
    scores = scores * TOK_DEV + lax.broadcasted_iota(jnp.int32, shape_all, 2)
    ranking = jnp.argsort(scores, axis=-1)
    return ranking[..., :SLOT].astype(jnp.int32)


def level_of(stream_key, dims, cuts, least, high):
    def one(axis_at, blocks):
        steps = jax.random.uniform(jax.random.fold_in(jax.random.fold_in(stream_key, 6), axis_at), (blocks,), jnp.float32, least / len(cuts), high / len(cuts))
        return jnp.repeat(jnp.exp(steps), dims[axis_at] // blocks).reshape((-1,) + (1,) * (len(dims) - axis_at - 1))

    level = one(*cuts[0])
    for cut in cuts[1:]:
        level = level * one(*cut)
    return level


def noise(key, extent, spread, limit, pieces=(), held_as=jnp.bfloat16):
    entries = jax.random.normal(key, extent, jnp.float32) * spread
    if len(pieces) > 0:
        entries = level_of(key, extent, pieces, -0.22, 0.18) * entries
    return jnp.clip(entries, min=-limit, max=limit).astype(held_as)


def setup_inputs(seed: int = 0, part: int = 0) -> dict:
    key_of = jax.random.split(jax.random.key(seed), 9)
    part_keys = jax.random.split(jax.random.fold_in(key_of[8], part), 9)
    tokens = draw_tokens(jax.random.fold_in(jax.random.fold_in(key_of[8], part), 71), part)
    pre_gain = jnp.clip(1.0 + 0.18 * jax.random.normal(key_of[1], (D,), jnp.float32), 0.1, 1.9)
    out_gain = jnp.clip(1.0 + 0.18 * jax.random.normal(key_of[2], (D,), jnp.float32), 0.1, 1.9)
    chosen = draw_chosen(jax.random.fold_in(jax.random.fold_in(key_of[8], part), 71), part)
    route_weight = jnp.clip(jnp.exp(math.log(3.0) - 2.3025851 * jax.random.uniform(part_keys[4], (BLOCKS, EXPERTS, SLOT), jnp.float32) ** level_of(part_keys[4], (BLOCKS, EXPERTS, SLOT), ((0, 4),), -0.2, 0.2)), 0.3, 3.0)
    expert_gate = noise(key_of[5], (EXPERTS, D, FF), D ** -0.5, 0.09375, ((0, 4), (2, 4)))
    expert_up = noise(key_of[6], (EXPERTS, D, FF), D ** -0.5, 0.09375, ((0, 4), (2, 4)))
    expert_down = noise(key_of[7], (EXPERTS, FF, D), FF ** -0.5, 0.109375, ((0, 4), (1, 4)))
    return dict(tokens=tokens, pre_gain=pre_gain, out_gain=out_gain, chosen=chosen, route_weight=route_weight, expert_gate=expert_gate, expert_up=expert_up, expert_down=expert_down)


NORM_EPS = 1e-06

def reference(tokens, pre_gain, out_gain, chosen, route_weight, expert_gate, expert_up, expert_down):
    resident = tokens.astype(jnp.float32)
    row_scale = lax.rsqrt(lax.optimization_barrier(jnp.mean(resident * resident, axis=1, keepdims=True)) + NORM_EPS)
    normed = (resident * row_scale * pre_gain).astype(jnp.bfloat16)
    offsets = (jnp.arange(BLOCKS, dtype=jnp.int32) * TOK_DEV)[:, None, None]
    global_index = jnp.transpose(chosen + offsets, (1, 0, 2)).reshape(EXPERTS, CAP).astype(jnp.int32)
    weights_flat = jnp.transpose(route_weight, (1, 0, 2)).reshape(EXPERTS, CAP)
    group_width = FF // N_TP

    def one_expert(operands):
        index_row, gate_matrix, up_matrix, down_matrix = operands
        picked_rows = jnp.take(normed, index_row, axis=0)
        gate_act = jnp.dot(picked_rows, gate_matrix, preferred_element_type=jnp.float32)
        up_act = jnp.dot(picked_rows, up_matrix, preferred_element_type=jnp.float32)
        hidden = (jax.nn.silu(gate_act) * up_act).astype(jnp.bfloat16)
        grouped = hidden.astype(jnp.float32).reshape(CAP, N_TP, group_width)
        down_groups = down_matrix.astype(jnp.float32).reshape(N_TP, group_width, D)
        partial_terms = jnp.einsum('cng,ngd->ncd', grouped, down_groups, precision=lax.Precision.HIGHEST).astype(jnp.bfloat16)
        partial_terms = lax.optimization_barrier(partial_terms)
        return lax.optimization_barrier(jnp.sum(partial_terms.astype(jnp.float32), axis=0)).astype(jnp.bfloat16)
    expert_out = lax.map(one_expert, (global_index, expert_gate, expert_up, expert_down))
    contributions = expert_out.astype(jnp.float32) * weights_flat[:, :, None]
    update = jnp.zeros((TOKENS, D), jnp.float32).at[global_index.reshape(-1)].add(contributions.reshape(-1, D))
    mixed_rows = resident + update
    out_scale = lax.rsqrt(lax.optimization_barrier(jnp.mean(mixed_rows * mixed_rows, axis=1, keepdims=True)) + NORM_EPS)
    return (mixed_rows * out_scale * out_gain).astype(jnp.bfloat16)
```

```python
import jax
import jax.numpy as jnp
from jax import lax
from jax.sharding import PartitionSpec as P

NORM_EPS = 1e-06
PRESCALE = 2.0 ** -20


def shift(value, axis, n, step):
    return lax.ppermute(value, axis, [(i, (i + step) % n) for i in range(n)])


def ring_gather(own, axis, n):
    half = own.shape[0] // 2
    forward, backward = own, own
    for d in range(1, n // 2 + 1):
        if 2 * d == n:
            forward = shift(forward[:half], axis, n, 1)
            backward = shift(backward[half:], axis, n, -1)
            yield d, jnp.concatenate([forward, backward], axis=0)
        else:
            forward = shift(forward, axis, n, 1)
            backward = shift(backward, axis, n, -1)
            yield -d, forward
            yield d, backward


def ring_scatter(part, axis, n, rows):
    half = rows // 2

    def add(full, extra, low):
        if extra is None:
            return full
        extra = extra.astype(jnp.float32)
        if extra.shape[0] == rows:
            return full + extra
        if low:
            return jnp.concatenate([full[:half] + extra, full[half:]], axis=0)
        return jnp.concatenate([full[:half], full[half:] + extra], axis=0)

    forward, backward = None, None
    for d in range(n // 2, 0, -1):
        if 2 * d == n:
            whole = part(d).astype(jnp.bfloat16)
            forward = shift(whole[:half], axis, n, 1)
            backward = shift(whole[half:], axis, n, -1)
        else:
            ahead = add(part(d), forward, True).astype(jnp.bfloat16)
            behind = add(part(-d), backward, False).astype(jnp.bfloat16)
            forward = shift(ahead, axis, n, 1)
            backward = shift(behind, axis, n, -1)
    return add(add(part(0), forward, True), backward, False)


def shards(tokens, pre_gain, out_gain, chosen, route_weight, expert_gate, expert_up, expert_down, n_ep, n_tp):
    model_width = pre_gain.shape[0]
    tok_count, shard_width = tokens.shape
    slot_count = chosen.shape[2]
    here_ep = lax.axis_index("ep")
    here_tp = lax.axis_index("tp")
    bf16, f32 = jnp.bfloat16, jnp.float32

    def relative(table):
        return lax.dynamic_slice_in_dim(jnp.concatenate([table, table], axis=0), here_ep, n_ep, 0)

    slots = relative(chosen[0]).reshape(-1)
    weights = relative(route_weight[0]).reshape(-1)
    token_ids = lax.broadcasted_iota(jnp.int32, (tok_count, slots.shape[0]), 0)
    hit = token_ids == slots[None, :]
    select = hit.astype(bf16)

    picked = lax.dot_general(
        select, tokens, (((0,), (0,)), ((), ())), preferred_element_type=f32
    ).astype(bf16)
    received = [picked[:slot_count]]
    for s in range(1, n_ep):
        received.append(shift(picked[s * slot_count:(s + 1) * slot_count], "ep", n_ep, s))
    rows = jnp.concatenate(received, axis=0)

    gate_matrix, up_matrix, down_matrix = expert_gate[0], expert_up[0], expert_down[0]

    def start_of(offset):
        return ((here_tp + offset) % n_tp) * shard_width

    def chunk(offset, block):
        start = start_of(offset)
        gain = lax.dynamic_slice_in_dim(pre_gain, start, shard_width, 0) * PRESCALE
        wide = block.astype(f32)
        squares = jnp.sum(wide * wide, axis=1)
        scaled = (wide * gain).astype(bf16)
        gate_rows = lax.dynamic_slice_in_dim(gate_matrix, start, shard_width, 0)
        up_rows = lax.dynamic_slice_in_dim(up_matrix, start, shard_width, 0)
        return (
            squares,
            jnp.dot(scaled, gate_rows, preferred_element_type=f32),
            jnp.dot(scaled, up_rows, preferred_element_type=f32),
        )

    square_sum, gate_act, up_act = chunk(0, rows)
    for offset, block in ring_gather(rows, "tp", n_tp):
        more = chunk(offset, block)
        square_sum, gate_act, up_act = square_sum + more[0], gate_act + more[1], up_act + more[2]
    row_scale = (lax.rsqrt(square_sum / model_width + NORM_EPS) / PRESCALE)[:, None]
    hidden = (jax.nn.silu(gate_act * row_scale) * (up_act * row_scale)).astype(bf16)

    def part(offset):
        columns = lax.dynamic_slice_in_dim(down_matrix, start_of(offset), shard_width, 1)
        return jnp.dot(hidden, columns, preferred_element_type=f32)

    expert_out = ring_scatter(part, "tp", n_tp, rows.shape[0]).astype(bf16)

    returned = [expert_out[:slot_count]]
    for s in range(1, n_ep):
        returned.append(shift(expert_out[s * slot_count:(s + 1) * slot_count], "ep", n_ep, -s))
    back = jnp.concatenate(returned, axis=0)

    spread = jnp.where(hit, weights[None, :], 0.0)
    coarse = spread.astype(bf16)
    fine = (spread - coarse.astype(f32)).astype(bf16)
    mixed = (
        tokens.astype(f32)
        + jnp.dot(coarse, back, preferred_element_type=f32)
        + jnp.dot(fine, back, preferred_element_type=f32)
    )
    own_sum = jnp.sum(mixed * mixed, axis=1)
    out_sum = own_sum
    for s in range(1, n_tp):
        out_sum = out_sum + shift(own_sum, "tp", n_tp, s)
    out_scale = lax.rsqrt(out_sum / model_width + NORM_EPS)[:, None]
    return (mixed * out_scale * out_gain).astype(bf16)


def solution(mesh):
    def body(*args):
        return shards(*args, n_ep=mesh.shape["ep"], n_tp=mesh.shape["tp"])

    return jax.shard_map(
        body,
        mesh=mesh,
        in_specs=(
            P(("grp", "ep"), "tp"),
            P(),
            P("tp"),
            P(("grp", "ep"), None, None),
            P(("grp", "ep"), None, None),
            P("ep", None, "tp"),
            P("ep", None, "tp"),
            P("ep", "tp", None),
        ),
        out_specs=P(("grp", "ep"), "tp"),
        check_vma=False,
    )
```

```python
import jax
import jax.numpy as jnp
from jax import lax
from jax.sharding import PartitionSpec as P

NORM_EPS = 1e-06
PRESCALE = 2.0 ** -20


def shift(value, axis, n, step):
    return lax.ppermute(value, axis, [(i, (i + step) % n) for i in range(n)])


def move(value, axis, pairs):
    return lax.ppermute(value, axis, pairs)


def line_gather(own, axis, n, here):
    right, left = own, own
    for k in range(1, n):
        going_right = [(i, i + 1) for i in range(k - 1, n - 1)]
        going_left = [(i, i - 1) for i in range(1, n - k + 1)]
        if k == n - 1 and n > 2:
            joined = jnp.where(here >= n // 2, right, left)
            arrived = move(joined, axis, going_right + going_left)
            yield [(jnp.where(here >= k, here - k, (here + k) % n), arrived)]
            continue
        right = move(right, axis, going_right)
        left = move(left, axis, going_left)
        if 2 * k >= n:
            yield [(jnp.where(here >= k, here - k, (here + k) % n), right + left)]
        else:
            yield [((here - k) % n, right), ((here + k) % n, left)]


def line_scatter(part, axis, n, here):
    bf16, f32 = jnp.bfloat16, jnp.float32
    right, left = None, None
    for d in range(n - 1, 0, -1):
        going_right = [(i, i + 1) for i in range(0, n - d)]
        going_left = [(i, i - 1) for i in range(d, n)]
        if 2 * d >= n:
            ahead = part(jnp.where(here < n - d, here + d, (here - d) % n))
            if right is not None:
                ahead = ahead + right.astype(f32) + left.astype(f32)
            ahead = ahead.astype(bf16)
            behind = ahead
        else:
            ahead, behind = part((here + d) % n), part((here - d) % n)
            if right is not None:
                ahead, behind = ahead + right.astype(f32), behind + left.astype(f32)
            ahead, behind = ahead.astype(bf16), behind.astype(bf16)
        if d == n - 1 and n > 2:
            both = move(ahead, axis, going_right + going_left)
            zero = jnp.zeros_like(both)
            right = jnp.where(here < n // 2, both, zero)
            left = jnp.where(here < n // 2, zero, both)
        else:
            right = move(ahead, axis, going_right)
            left = move(behind, axis, going_left)
    total = part(here)
    if right is None:
        return total
    return total + right.astype(f32) + left.astype(f32)


def shards(tokens, pre_gain, out_gain, chosen, route_weight, expert_gate, expert_up, expert_down, n_ep, n_tp):
    model_width = pre_gain.shape[0]
    tok_count, shard_width = tokens.shape
    slot_count = chosen.shape[2]
    here_ep = lax.axis_index("ep")
    here_tp = lax.axis_index("tp")
    bf16, f32 = jnp.bfloat16, jnp.float32

    def relative(table):
        return lax.dynamic_slice_in_dim(jnp.concatenate([table, table], axis=0), here_ep, n_ep, 0)

    slots = relative(chosen[0]).reshape(-1)
    weights = relative(route_weight[0]).reshape(-1)
    token_ids = lax.broadcasted_iota(jnp.int32, (tok_count, slots.shape[0]), 0)
    hit = token_ids == slots[None, :]
    select = hit.astype(bf16)

    picked = lax.dot_general(
        select, tokens, (((0,), (0,)), ((), ())), preferred_element_type=f32
    ).astype(bf16)
    received = [picked[:slot_count]]
    for s in range(1, n_ep):
        received.append(shift(picked[s * slot_count:(s + 1) * slot_count], "ep", n_ep, s))

    gate_matrix, up_matrix, down_matrix = expert_gate[0], expert_up[0], expert_down[0]

    def chunk(owner, block):
        start = owner * shard_width
        gain = lax.dynamic_slice_in_dim(pre_gain, start, shard_width, 0) * PRESCALE
        wide = block.astype(f32)
        squares = jnp.sum(wide * wide, axis=1)
        scaled = (wide * gain).astype(bf16)
        gate_rows = lax.dynamic_slice_in_dim(gate_matrix, start, shard_width, 0)
        up_rows = lax.dynamic_slice_in_dim(up_matrix, start, shard_width, 0)
        return (
            squares,
            jnp.dot(scaled, gate_rows, preferred_element_type=f32),
            jnp.dot(scaled, up_rows, preferred_element_type=f32),
        )

    def gathered(rows):
        total = chunk(here_tp, rows)
        marks = [rows]
        for arrivals in line_gather(rows, "tp", n_tp, here_tp):
            for owner, block in arrivals:
                total = tuple(x + y for x, y in zip(total, chunk(owner, block)))
            marks.append(arrivals[-1][1])
        square_sum, gate_act, up_act = total
        row_scale = (lax.rsqrt(square_sum / model_width + NORM_EPS) / PRESCALE)[:, None]
        hidden = (jax.nn.silu(gate_act * row_scale) * (up_act * row_scale)).astype(bf16)
        return hidden, marks[-2] if len(marks) > 1 else rows

    def part_of(hidden):
        def part(owner):
            columns = lax.dynamic_slice_in_dim(down_matrix, owner * shard_width, shard_width, 1)
            return jnp.dot(hidden, columns, preferred_element_type=f32)

        return part

    cut = (n_ep + 1) // 2
    returned = []
    mark = None
    for group in (range(0, cut), range(cut, n_ep)):
        if len(group) == 0:
            continue
        rows = jnp.concatenate([received[s] for s in group], axis=0)
        if mark is not None:
            rows, _ = lax.optimization_barrier((rows, mark))
        hidden, mark = gathered(rows)
        expert_out = line_scatter(part_of(hidden), "tp", n_tp, here_tp).astype(bf16)
        for at, s in enumerate(group):
            piece = expert_out[at * slot_count:(at + 1) * slot_count]
            returned.append(shift(piece, "ep", n_ep, -s) if s else piece)
    back = jnp.concatenate(returned, axis=0)

    spread = jnp.where(hit, weights[None, :], 0.0)
    coarse = spread.astype(bf16)
    fine = (spread - coarse.astype(f32)).astype(bf16)
    mixed = (
        tokens.astype(f32)
        + jnp.dot(coarse, back, preferred_element_type=f32)
        + jnp.dot(fine, back, preferred_element_type=f32)
    )
    own_sum = jnp.sum(mixed * mixed, axis=1)
    out_sum = own_sum
    for s in range(1, n_tp):
        out_sum = out_sum + shift(own_sum, "tp", n_tp, s)
    out_scale = lax.rsqrt(out_sum / model_width + NORM_EPS)[:, None]
    return (mixed * out_scale * out_gain).astype(bf16)


def solution(mesh):
    def body(*args):
        return shards(*args, n_ep=mesh.shape["ep"], n_tp=mesh.shape["tp"])

    return jax.shard_map(
        body,
        mesh=mesh,
        in_specs=(
            P(("grp", "ep"), "tp"),
            P(),
            P("tp"),
            P(("grp", "ep"), None, None),
            P(("grp", "ep"), None, None),
            P("ep", None, "tp"),
            P("ep", None, "tp"),
            P("ep", "tp", None),
        ),
        out_specs=P(("grp", "ep"), "tp"),
        check_vma=False,
    )
```

```python
import jax
import jax.numpy as jnp
from jax import lax
from jax.sharding import PartitionSpec as P

NORM_EPS = 1e-06
PRESCALE = 2.0 ** -20


def shift(value, axis, n, step):
    return lax.ppermute(value, axis, [(i, (i + step) % n) for i in range(n)])


def ring_gather(own, axis, n):
    half = own.shape[0] // 2
    forward, backward = own, own
    for d in range(1, n // 2 + 1):
        if 2 * d == n:
            forward = shift(forward[:half], axis, n, 1)
            backward = shift(backward[half:], axis, n, -1)
            yield d, jnp.concatenate([forward, backward], axis=0)
        else:
            forward = shift(forward, axis, n, 1)
            backward = shift(backward, axis, n, -1)
            yield -d, forward
            yield d, backward


def ring_scatter(part, axis, n, rows):
    half = rows // 2
    parts = {}

    def take(offset, low):
        if offset not in parts:
            parts[offset] = part(offset)
        return parts[offset][:half] if low else parts[offset][half:]

    arrived = {}
    for d in range(n // 2, 0, -1):
        for low, way in ((True, 1), (False, -1), (False, 1), (True, -1)):
            if 2 * d == n and low != (way == 1):
                continue
            value = take(way * d if 2 * d < n else d, low)
            if (low, way) in arrived:
                value = value + arrived[low, way].astype(jnp.float32)
            arrived[low, way] = shift(value.astype(jnp.bfloat16), axis, n, way)
    sums = []
    for low in (True, False):
        value = take(0, low)
        for way in (1, -1):
            if (low, way) in arrived:
                value = value + arrived[low, way].astype(jnp.float32)
        sums.append(value)
    return jnp.concatenate(sums, axis=0)


def shards(tokens, pre_gain, out_gain, chosen, route_weight, expert_gate, expert_up, expert_down, n_ep, n_tp):
    model_width = pre_gain.shape[0]
    tok_count, shard_width = tokens.shape
    slot_count = chosen.shape[2]
    here_ep = lax.axis_index("ep")
    here_tp = lax.axis_index("tp")
    bf16, f32 = jnp.bfloat16, jnp.float32

    def relative(table):
        return lax.dynamic_slice_in_dim(jnp.concatenate([table, table], axis=0), here_ep, n_ep, 0)

    slots = relative(chosen[0]).reshape(-1)
    weights = relative(route_weight[0]).reshape(-1)
    token_ids = lax.broadcasted_iota(jnp.int32, (tok_count, slots.shape[0]), 0)
    hit = token_ids == slots[None, :]

    def pick(s):
        ids = slots[s * slot_count:(s + 1) * slot_count]
        select = (ids[:, None] == lax.broadcasted_iota(jnp.int32, (slot_count, tok_count), 1)).astype(bf16)
        return jnp.dot(select, tokens, preferred_element_type=f32).astype(bf16)

    received = [shift(pick(s), "ep", n_ep, s) for s in range(n_ep - 1, 0, -1)][::-1]
    received = [pick(0)] + received
    rows = jnp.concatenate(received, axis=0)

    gate_matrix, up_matrix, down_matrix = expert_gate[0], expert_up[0], expert_down[0]

    def start_of(offset):
        return ((here_tp + offset) % n_tp) * shard_width

    def chunk(offset, block):
        start = start_of(offset)
        gain = lax.dynamic_slice_in_dim(pre_gain, start, shard_width, 0) * PRESCALE
        wide = block.astype(f32)
        squares = jnp.sum(wide * wide, axis=1)
        scaled = (wide * gain).astype(bf16)
        gate_rows = lax.dynamic_slice_in_dim(gate_matrix, start, shard_width, 0)
        up_rows = lax.dynamic_slice_in_dim(up_matrix, start, shard_width, 0)
        return (
            squares,
            jnp.dot(scaled, gate_rows, preferred_element_type=f32),
            jnp.dot(scaled, up_rows, preferred_element_type=f32),
        )

    square_sum, gate_act, up_act = chunk(0, rows)
    for offset, block in ring_gather(rows, "tp", n_tp):
        block, square_sum, gate_act, up_act = lax.optimization_barrier((block, square_sum, gate_act, up_act))
        more = chunk(offset, block)
        square_sum, gate_act, up_act = square_sum + more[0], gate_act + more[1], up_act + more[2]
    row_scale = (lax.rsqrt(square_sum / model_width + NORM_EPS) / PRESCALE)[:, None]
    hidden = (jax.nn.silu(gate_act * row_scale) * (up_act * row_scale)).astype(bf16)

    def part(offset):
        columns = lax.dynamic_slice_in_dim(down_matrix, start_of(offset), shard_width, 1)
        return jnp.dot(hidden, columns, preferred_element_type=f32)

    expert_out = ring_scatter(part, "tp", n_tp, rows.shape[0]).astype(bf16)

    returned = [expert_out[:slot_count]]
    for s in range(1, n_ep):
        returned.append(shift(expert_out[s * slot_count:(s + 1) * slot_count], "ep", n_ep, -s))
    back = jnp.concatenate(returned, axis=0)

    spread = jnp.where(hit, weights[None, :], 0.0)
    coarse = spread.astype(bf16)
    fine = (spread - coarse.astype(f32)).astype(bf16)
    mixed = (
        tokens.astype(f32)
        + jnp.dot(coarse, back, preferred_element_type=f32)
        + jnp.dot(fine, back, preferred_element_type=f32)
    )
    own_sum = jnp.sum(mixed * mixed, axis=1)
    out_sum = own_sum
    if n_tp & (n_tp - 1) == 0:
        bit = 1
        while bit < n_tp:
            out_sum = out_sum + lax.ppermute(out_sum, "tp", [(i, i ^ bit) for i in range(n_tp)])
            bit *= 2
    else:
        for s in range(1, n_tp):
            out_sum = out_sum + shift(own_sum, "tp", n_tp, s)
    out_scale = lax.rsqrt(out_sum / model_width + NORM_EPS)[:, None]
    return (mixed * out_scale * out_gain).astype(bf16)


def solution(mesh):
    def body(*args):
        return shards(*args, n_ep=mesh.shape["ep"], n_tp=mesh.shape["tp"])

    return jax.shard_map(
        body,
        mesh=mesh,
        in_specs=(
            P(("grp", "ep"), "tp"),
            P(),
            P("tp"),
            P(("grp", "ep"), None, None),
            P(("grp", "ep"), None, None),
            P("ep", None, "tp"),
            P("ep", None, "tp"),
            P("ep", "tp", None),
        ),
        out_specs=P(("grp", "ep"), "tp"),
        check_vma=False,
    )
```

```python
import jax
import jax.numpy as jnp
from jax import lax
from jax.sharding import PartitionSpec as P

NORM_EPS = 1e-06
PRESCALE = 2.0 ** -20


def shift(value, axis, n, step):
    return lax.ppermute(value, axis, [(i, (i + step) % n) for i in range(n)])


def ring_gather(own, axis, n):
    half = own.shape[0] // 2
    forward, backward = own, own
    for d in range(1, n // 2 + 1):
        if 2 * d == n:
            forward = shift(forward[:half], axis, n, 1)
            backward = shift(backward[half:], axis, n, -1)
            yield d, jnp.concatenate([forward, backward], axis=0)
        else:
            forward = shift(forward, axis, n, 1)
            backward = shift(backward, axis, n, -1)
            yield -d, forward
            yield d, backward


def ring_scatter(part, axis, n, rows):
    half = rows // 2

    def add(full, extra, low):
        if extra is None:
            return full
        extra = extra.astype(jnp.float32)
        if extra.shape[0] == rows:
            return full + extra
        if low:
            return jnp.concatenate([full[:half] + extra, full[half:]], axis=0)
        return jnp.concatenate([full[:half], full[half:] + extra], axis=0)

    forward, backward = None, None
    for d in range(n // 2, 0, -1):
        if 2 * d == n:
            whole = part(d).astype(jnp.bfloat16)
            forward = shift(whole[:half], axis, n, 1)
            backward = shift(whole[half:], axis, n, -1)
        else:
            ahead = add(part(d), forward, True).astype(jnp.bfloat16)
            behind = add(part(-d), backward, False).astype(jnp.bfloat16)
            forward = shift(ahead, axis, n, 1)
            backward = shift(behind, axis, n, -1)
    return add(add(part(0), forward, True), backward, False)


def shards(tokens, pre_gain, out_gain, chosen, route_weight, expert_gate, expert_up, expert_down, n_ep, n_tp):
    model_width = pre_gain.shape[0]
    tok_count, shard_width = tokens.shape
    slot_count = chosen.shape[2]
    here_ep = lax.axis_index("ep")
    here_tp = lax.axis_index("tp")
    bf16, f32 = jnp.bfloat16, jnp.float32

    def relative(table):
        return lax.dynamic_slice_in_dim(jnp.concatenate([table, table], axis=0), here_ep, n_ep, 0)

    slots = relative(chosen[0]).reshape(-1)
    weights = relative(route_weight[0]).reshape(-1)
    token_ids = lax.broadcasted_iota(jnp.int32, (tok_count, slots.shape[0]), 0)
    hit = token_ids == slots[None, :]
    select = hit.astype(bf16)

    picked = lax.dot_general(
        select, tokens, (((0,), (0,)), ((), ())), preferred_element_type=f32
    ).astype(bf16)
    received = [picked[:slot_count]]
    for s in range(1, n_ep):
        received.append(shift(picked[s * slot_count:(s + 1) * slot_count], "ep", n_ep, s))
    rows = jnp.concatenate(received, axis=0)

    gate_matrix, up_matrix, down_matrix = expert_gate[0], expert_up[0], expert_down[0]

    def start_of(offset):
        return ((here_tp + offset) % n_tp) * shard_width

    def chunk(offset, block):
        start = start_of(offset)
        gain = lax.dynamic_slice_in_dim(pre_gain, start, shard_width, 0) * PRESCALE
        wide = block.astype(f32)
        squares = jnp.sum(wide * wide, axis=1)
        scaled = (wide * gain).astype(bf16)
        gate_rows = lax.dynamic_slice_in_dim(gate_matrix, start, shard_width, 0)
        up_rows = lax.dynamic_slice_in_dim(up_matrix, start, shard_width, 0)
        return (
            squares,
            jnp.dot(scaled, gate_rows, preferred_element_type=f32),
            jnp.dot(scaled, up_rows, preferred_element_type=f32),
        )

    square_sum, gate_act, up_act = chunk(0, rows)
    for offset, block in ring_gather(rows, "tp", n_tp):
        if 2 * offset == n_tp:
            block, square_sum, gate_act, up_act = lax.optimization_barrier((block, square_sum, gate_act, up_act))
        more = chunk(offset, block)
        square_sum, gate_act, up_act = square_sum + more[0], gate_act + more[1], up_act + more[2]
    row_scale = (lax.rsqrt(square_sum / model_width + NORM_EPS) / PRESCALE)[:, None]
    hidden = (jax.nn.silu(gate_act * row_scale) * (up_act * row_scale)).astype(bf16)

    def part(offset):
        columns = lax.dynamic_slice_in_dim(down_matrix, start_of(offset), shard_width, 1)
        return jnp.dot(hidden, columns, preferred_element_type=f32)

    expert_out = ring_scatter(part, "tp", n_tp, rows.shape[0]).astype(bf16)

    returned = [expert_out[:slot_count]]
    for s in range(1, n_ep):
        returned.append(shift(expert_out[s * slot_count:(s + 1) * slot_count], "ep", n_ep, -s))
    back = jnp.concatenate(returned, axis=0)

    spread = jnp.where(hit, weights[None, :], 0.0)
    coarse = spread.astype(bf16)
    fine = (spread - coarse.astype(f32)).astype(bf16)
    mixed = (
        tokens.astype(f32)
        + jnp.dot(coarse, back, preferred_element_type=f32)
        + jnp.dot(fine, back, preferred_element_type=f32)
    )
    own_sum = jnp.sum(mixed * mixed, axis=1)
    out_sum = own_sum
    for s in range(1, n_tp):
        out_sum = out_sum + shift(own_sum, "tp", n_tp, s)
    out_scale = lax.rsqrt(out_sum / model_width + NORM_EPS)[:, None]
    return (mixed * out_scale * out_gain).astype(bf16)


def solution(mesh):
    def body(*args):
        return shards(*args, n_ep=mesh.shape["ep"], n_tp=mesh.shape["tp"])

    return jax.shard_map(
        body,
        mesh=mesh,
        in_specs=(
            P(("grp", "ep"), "tp"),
            P(),
            P("tp"),
            P(("grp", "ep"), None, None),
            P(("grp", "ep"), None, None),
            P("ep", None, "tp"),
            P("ep", None, "tp"),
            P("ep", "tp", None),
        ),
        out_specs=P(("grp", "ep"), "tp"),
        check_vma=False,
    )
```

```python
import jax
import jax.numpy as jnp
from jax import lax
from jax.sharding import PartitionSpec as P

NORM_EPS = 1e-06
PRESCALE = 2.0 ** -20


def shift(value, axis, n, step):
    return lax.ppermute(value, axis, [(i, (i + step) % n) for i in range(n)])


def ring_gather(own, axis, n):
    half = own.shape[0] // 2
    forward, backward = own, own
    for d in range(1, n // 2 + 1):
        if 2 * d == n:
            forward = shift(forward[:half], axis, n, 1)
            backward = shift(backward[half:], axis, n, -1)
            yield d, jnp.concatenate([forward, backward], axis=0)
        else:
            forward = shift(forward, axis, n, 1)
            backward = shift(backward, axis, n, -1)
            yield -d, forward
            yield d, backward


def ring_scatter(part, axis, n, rows):
    half = rows // 2

    def add(full, extra, low):
        if extra is None:
            return full
        extra = extra.astype(jnp.float32)
        if extra.shape[0] == rows:
            return full + extra
        if low:
            return jnp.concatenate([full[:half] + extra, full[half:]], axis=0)
        return jnp.concatenate([full[:half], full[half:] + extra], axis=0)

    forward, backward = None, None
    for d in range(n // 2, 0, -1):
        if 2 * d == n:
            whole = part(d).astype(jnp.bfloat16)
            forward = shift(whole[:half], axis, n, 1)
            backward = shift(whole[half:], axis, n, -1)
        else:
            ahead = add(part(d), forward, True).astype(jnp.bfloat16)
            behind = add(part(-d), backward, False).astype(jnp.bfloat16)
            forward = shift(ahead, axis, n, 1)
            backward = shift(behind, axis, n, -1)
    return add(add(part(0), forward, True), backward, False)


def shards(tokens, pre_gain, out_gain, chosen, route_weight, expert_gate, expert_up, expert_down, n_ep, n_tp):
    model_width = pre_gain.shape[0]
    tok_count, shard_width = tokens.shape
    slot_count = chosen.shape[2]
    here_ep = lax.axis_index("ep")
    here_tp = lax.axis_index("tp")
    bf16, f32 = jnp.bfloat16, jnp.float32

    def relative(table):
        wanted = (here_ep + lax.broadcasted_iota(jnp.int32, (n_ep, n_ep, 1), 0)) % n_ep
        own = wanted == lax.broadcasted_iota(jnp.int32, (n_ep, n_ep, 1), 1)
        return jnp.sum(jnp.where(own, table[None], jnp.zeros_like(table)[None]), axis=1)

    slots = relative(chosen[0]).reshape(-1)
    weights = relative(route_weight[0]).reshape(-1)
    token_ids = lax.broadcasted_iota(jnp.int32, (tok_count, slots.shape[0]), 0)
    hit = token_ids == slots[None, :]
    select = hit.astype(bf16)

    picked = lax.dot_general(
        select, tokens, (((0,), (0,)), ((), ())), preferred_element_type=f32
    ).astype(bf16)
    received = [picked[:slot_count]]
    for s in range(1, n_ep):
        received.append(shift(picked[s * slot_count:(s + 1) * slot_count], "ep", n_ep, s))
    rows = jnp.concatenate(received, axis=0)

    gate_matrix, up_matrix, down_matrix = expert_gate[0], expert_up[0], expert_down[0]

    def start_of(offset):
        return ((here_tp + offset) % n_tp) * shard_width

    def chunk(offset, block):
        start = start_of(offset)
        gain = lax.dynamic_slice_in_dim(pre_gain, start, shard_width, 0) * PRESCALE
        wide = block.astype(f32)
        squares = jnp.sum(wide * wide, axis=1)
        scaled = (wide * gain).astype(bf16)
        gate_rows = lax.dynamic_slice_in_dim(gate_matrix, start, shard_width, 0)
        up_rows = lax.dynamic_slice_in_dim(up_matrix, start, shard_width, 0)
        return (
            squares,
            jnp.dot(scaled, gate_rows, preferred_element_type=f32),
            jnp.dot(scaled, up_rows, preferred_element_type=f32),
        )

    square_sum, gate_act, up_act = chunk(0, rows)
    for offset, block in ring_gather(rows, "tp", n_tp):
        if 2 * offset == n_tp:
            block, square_sum, gate_act, up_act = lax.optimization_barrier((block, square_sum, gate_act, up_act))
        more = chunk(offset, block)
        square_sum, gate_act, up_act = square_sum + more[0], gate_act + more[1], up_act + more[2]
    row_scale = (lax.rsqrt(square_sum / model_width + NORM_EPS) / PRESCALE)[:, None]
    hidden = (jax.nn.silu(gate_act * row_scale) * (up_act * row_scale)).astype(bf16)

    def part(offset):
        columns = lax.dynamic_slice_in_dim(down_matrix, start_of(offset), shard_width, 1)
        return jnp.dot(hidden, columns, preferred_element_type=f32)

    expert_out = ring_scatter(part, "tp", n_tp, rows.shape[0]).astype(bf16)

    returned = [expert_out[:slot_count]]
    for s in range(1, n_ep):
        returned.append(shift(expert_out[s * slot_count:(s + 1) * slot_count], "ep", n_ep, -s))
    back = jnp.concatenate(returned, axis=0)

    spread = jnp.where(hit, weights[None, :], 0.0)
    coarse = spread.astype(bf16)
    fine = (spread - coarse.astype(f32)).astype(bf16)
    mixed = (
        tokens.astype(f32)
        + jnp.dot(coarse, back, preferred_element_type=f32)
        + jnp.dot(fine, back, preferred_element_type=f32)
    )
    own_sum = jnp.sum(mixed * mixed, axis=1)
    out_sum = own_sum
    for s in range(1, n_tp):
        out_sum = out_sum + shift(own_sum, "tp", n_tp, s)
    out_scale = lax.rsqrt(out_sum / model_width + NORM_EPS)[:, None]
    return (mixed * out_scale * out_gain).astype(bf16)


def solution(mesh):
    def body(*args):
        return shards(*args, n_ep=mesh.shape["ep"], n_tp=mesh.shape["tp"])

    return jax.shard_map(
        body,
        mesh=mesh,
        in_specs=(
            P(("grp", "ep"), "tp"),
            P(),
            P("tp"),
            P(("grp", "ep"), None, None),
            P(("grp", "ep"), None, None),
            P("ep", None, "tp"),
            P("ep", None, "tp"),
            P("ep", "tp", None),
        ),
        out_specs=P(("grp", "ep"), "tp"),
        check_vma=False,
    )
```
